32 devices in a mesh: grp: 2 (over y), sp: 4 (over z), tp: 4 (over x, core).
Axes of the slice: x: 2, y: 2, z: 4, core: 2. Of those that a mesh axis runs over, the one named last changes fastest.
Arguments:
- query_first: bfloat16 [1536, 512], P(('grp', 'sp'), 'tp'), parts along dimension 0, may hold values from -172 to 172
- key_first: bfloat16 [1536, 512], P(('grp', 'sp'), 'tp'), parts along dimension 0, may hold values from -7.8 to 7.8
- query_second: bfloat16 [1536, 1024], P(('grp', 'sp'), 'tp'), parts along dimension 0, may hold values from -172 to 172
- key_second: bfloat16 [1536, 1024], P(('grp', 'sp'), 'tp'), parts along dimension 0, may hold values from -7.8 to 7.8
- values: bfloat16 [1536, 2, 512], P(('grp', 'sp'), None, 'tp'), parts along dimension 0, may hold values from -6 to 6
- lambdas: float32 [2, 4], P(None, 'tp'), may hold values from 0.3 to 0.8
- residual: bfloat16 [1536, 2048], P(('grp', 'sp'), 'tp'), parts along dimension 0, may hold values from -130 to 130
- norm_gain: bfloat16 [2048], P('tp'), may hold values from 0.099609375 to 1.8984375
- out_weight: bfloat16 [2, 512, 2048], P(None, 'tp'), may hold values from -0.1875 to 0.1875
- gate_weight: bfloat16 [2048, 5632], P('sp', 'tp'), may hold values from -0.125 to 0.125
- up_weight: bfloat16 [2048, 5632], P('sp', 'tp'), may hold values from -0.125 to 0.125
- down_weight: bfloat16 [5632, 2048], P('tp', 'sp'), may hold values from -0.078125 to 0.078125
Outputs:
- layer_out: bfloat16 [1536, 2048], P(('grp', 'sp'), 'tp'), parts along dimension 0
The draws below stay inside these ranges and needn't reach their ends.
There are 2 independent parts, one for each index of `grp`. The reference program is written for one: setup_inputs(seed, part) draws one part's arguments, and reference() takes and returns one part's arrays. A program takes and returns all parts, laid end to end along the dimension named above; an argument that names none is the same for every part. Nothing has to cross between parts.
All inputs are finite; a program needn't handle non-finite values.
Results may differ from the reference program's by a relative error of at most 0.0065.
Values may be sent and summed in bfloat16 or wider, within the bound.
No kernel may reach another device: no remote copies, remote signals or barrier semaphores. Data moves between devices by JAX's collectives and lax.ppermute only.
A program may use at most 128 MiB of HBM per device.

```python
import jax
import jax.numpy as jnp
from jax import lax

D = 2048
FF = 5632
HEADS = 4
DKA = 64
DKB = 128
DV = 128
SEQ = 768


def paired_draw(key, salt, key_width):
    base = jax.random.fold_in(key, salt)
    key_draw = jax.random.normal(jax.random.fold_in(base, 1), (SEQ, HEADS * 2 * key_width), jnp.float32)
    query_draw = jax.random.normal(jax.random.fold_in(base, 2), (SEQ, HEADS * 2 * key_width), jnp.float32)
    keys_out = 1.3 * jnp.clip(key_draw, -6.0, 6.0)
    queries_out = 1.3 * jnp.clip(query_draw, -6.0, 6.0)
    return (queries_out, keys_out)


def draw_query_first(key, part):
    return paired_draw(key, 11, DKA)[0].astype(jnp.bfloat16)


def draw_key_first(key, part):
    return paired_draw(key, 11, DKA)[1].astype(jnp.bfloat16)


def draw_query_second(key, part):
    return paired_draw(key, 23, DKB)[0].astype(jnp.bfloat16)


def draw_key_second(key, part):
    return paired_draw(key, 23, DKB)[1].astype(jnp.bfloat16)


def draw_residual(key, part):
    base = jax.random.fold_in(key, 37)
    entries = jnp.clip(jax.random.normal(jax.random.fold_in(base, 1), (SEQ, D), jnp.float32), -6.0, 6.0)
    jitter = jnp.clip(jax.random.normal(jax.random.fold_in(base, 2), (1, D), jnp.float32), -2.0, 2.0)
    column = 0.3 * 10.0 ** (jnp.arange(D, dtype=jnp.float32)[None, :] / D + 0.1 * jitter)
    row_scale = 0.3 * 10.0 ** jax.random.uniform(jax.random.fold_in(base, 3), (SEQ, 1), jnp.float32)
    result = entries * column * row_scale
    return result.astype(jnp.bfloat16)


def block_scale(rng, dims, pieces, low, top_value):
    def one(axis_at, parts):
        heights = jax.random.uniform(jax.random.fold_in(jax.random.fold_in(rng, 6), axis_at), (parts,), jnp.float32, low / len(pieces), top_value / len(pieces))
        return jnp.repeat(jnp.exp(heights), dims[axis_at] // parts).reshape((-1,) + (1,) * (len(dims) - axis_at - 1))

    factor_of = one(*pieces[0])
    for cut in pieces[1:]:
        factor_of = factor_of * one(*cut)
    return factor_of


def bell_draw(rng, shape, spread, reach, pieces=(), held_as=jnp.bfloat16):
    values = jax.random.normal(rng, shape, jnp.float32) * spread
    if len(pieces) > 0:
        values = block_scale(rng, shape, pieces, -0.22, 0.18) * values
    return jnp.clip(values, min=-reach, max=reach).astype(held_as)


def setup_inputs(seed: int = 0, part: int = 0) -> dict:
    seeds = jax.random.split(jax.random.key(seed), 13)
    own_keys = jax.random.split(jax.random.fold_in(seeds[12], part), 13)
    query_first = draw_query_first(jax.random.fold_in(jax.random.fold_in(seeds[12], part), 71), part)
    key_first = draw_key_first(jax.random.fold_in(jax.random.fold_in(seeds[12], part), 71), part)
    query_second = draw_query_second(jax.random.fold_in(jax.random.fold_in(seeds[12], part), 71), part)
    key_second = draw_key_second(jax.random.fold_in(jax.random.fold_in(seeds[12], part), 71), part)
    values = bell_draw(own_keys[4], (SEQ, 2, HEADS * DV), 1.0, 6.0, ((0, 4), (2, 4)))
    lambdas = jnp.clip(0.3 + 0.5 * jax.random.uniform(seeds[5], (2, HEADS), jnp.float32) ** block_scale(seeds[5], (2, HEADS), ((1, 4),), -0.2, 0.2), 0.3, 0.8)
    residual = draw_residual(jax.random.fold_in(jax.random.fold_in(seeds[12], part), 71), part)
    norm_gain = jnp.clip(1.0 + 0.18 * jax.random.normal(seeds[7], (D,), jnp.float32), 0.099609375, 1.8984375).astype(jnp.bfloat16)
    out_weight = bell_draw(seeds[8], (2, HEADS * DV, D), (2 * HEADS * DV) ** -0.5, 0.1875, ((1, 4),))
    gate_weight = bell_draw(seeds[9], (D, FF), D ** -0.5, 0.125, ((0, 4), (1, 4)))
    up_weight = bell_draw(seeds[10], (D, FF), D ** -0.5, 0.125, ((0, 4), (1, 4)))
    down_weight = bell_draw(seeds[11], (FF, D), FF ** -0.5, 0.078125, ((0, 4), (1, 4)))
    return dict(query_first=query_first, key_first=key_first, query_second=query_second, key_second=key_second, values=values, lambdas=lambdas, residual=residual, norm_gain=norm_gain, out_weight=out_weight, gate_weight=gate_weight, up_weight=up_weight, down_weight=down_weight)


def one_head(query_rows, key_rows, value_rows, lam_value, key_width):
    block_rows = 512 if SEQ % 512 == 0 else SEQ
    blocks = SEQ // block_rows
    query_blocks = query_rows.reshape(blocks, block_rows, 2, key_width)
    starts = jnp.arange(blocks, dtype=jnp.int32) * block_rows
    key_pos = jnp.arange(SEQ, dtype=jnp.int32)[None, :]
    key_f32 = key_rows.astype(jnp.float32)
    value_f32 = value_rows.astype(jnp.float32)

    def per_block(inputs):
        query_block, offset = inputs
        query_pos = offset + jnp.arange(block_rows, dtype=jnp.int32)[:, None]
        allowed = key_pos <= query_pos
        scores = jnp.einsum('qmd,kmd->mqk', query_block.astype(jnp.float32), key_f32) * key_width ** (-0.5)
        scores = jnp.where(allowed, scores, -1e+30)
        peak = lax.optimization_barrier(jnp.max(scores, axis=-1, keepdims=True))
        weights = jnp.where(allowed, jnp.exp(scores - peak), 0.0)
        totals = lax.optimization_barrier(jnp.sum(weights, axis=-1, keepdims=True))
        rounded = weights.astype(jnp.bfloat16).astype(jnp.float32)
        map_out = jnp.einsum('mqk,ke->mqe', rounded, value_f32) / totals
        differ = map_out[0] - lam_value * map_out[1]
        scale = lax.rsqrt(lax.optimization_barrier(jnp.mean(differ * differ, axis=-1, keepdims=True)) + 1e-06)
        return (0.8 * differ * scale).astype(jnp.bfloat16)
    result = lax.map(per_block, (query_blocks, starts))
    return result.reshape(SEQ, DV)

def reference(query_first, key_first, query_second, key_second, values, lambdas, residual, norm_gain, out_weight, gate_weight, up_weight, down_weight):
    mixed = jnp.zeros((SEQ, D), jnp.float32)
    groups = ((query_first, key_first, DKA), (query_second, key_second, DKB))
    for group_idx in range(2):
        query_all, key_all, key_width = groups[group_idx]
        query_heads = query_all.reshape(SEQ, HEADS, 2, key_width)
        key_heads = key_all.reshape(SEQ, HEADS, 2, key_width)
        value_heads = values[:, group_idx].reshape(SEQ, HEADS, DV)
        outputs = []
        for head in range(HEADS):
            outputs.append(one_head(query_heads[:, head], key_heads[:, head], value_heads[:, head], lambdas[group_idx, head], key_width))
        attended = jnp.concatenate(outputs, axis=1)
        mixed = mixed + jnp.dot(attended, out_weight[group_idx], preferred_element_type=jnp.float32)
    stream = residual.astype(jnp.float32) + mixed
    scale = lax.rsqrt(lax.optimization_barrier(jnp.mean(stream * stream, axis=1, keepdims=True)) + 1e-06)
    normed = (stream * scale * norm_gain.astype(jnp.float32)).astype(jnp.bfloat16)
    gate = jnp.dot(normed, gate_weight, preferred_element_type=jnp.float32)
    up_part = jnp.dot(normed, up_weight, preferred_element_type=jnp.float32)
    hidden = (jax.nn.silu(gate) * up_part).astype(jnp.bfloat16)
    ffn = jnp.dot(hidden, down_weight, preferred_element_type=jnp.float32)
    return (stream + 0.5 * ffn).astype(jnp.bfloat16)
```

```python
import jax
import jax.numpy as jnp
from jax import lax
from jax.sharding import PartitionSpec as P

D = 2048


def gathered_weights(
    query_first,
    key_first,
    query_second,
    key_second,
    values,
    lambdas,
    residual,
    norm_gain,
    out_weight,
    gate_weight,
    up_weight,
    down_weight,
):
    tok_rows = query_first.shape[0]
    heads_here = lambdas.shape[1]
    width_first = query_first.shape[1] // (2 * heads_here)
    width_second = query_second.shape[1] // (2 * heads_here)
    value_size = values.shape[2] // heads_here
    offset = lax.axis_index("sp") * tok_rows
    query_pos = offset + lax.broadcasted_iota(jnp.int32, (tok_rows, 1), 0)
    query_groups = (
        query_first.reshape(tok_rows, heads_here, 2, width_first),
        query_second.reshape(tok_rows, heads_here, 2, width_second),
    )
    key_widths = (width_first, width_second)
    start_state = (
        jnp.full((heads_here, 2, tok_rows, 1), -1e30, jnp.float32),
        jnp.zeros((heads_here, 2, tok_rows, 1), jnp.float32),
        jnp.zeros((heads_here, 2, tok_rows, value_size), jnp.float32),
    )
    states = (start_state, start_state)
    pieces = (
        lax.all_gather(key_first, "sp", axis=0, tiled=True),
        lax.all_gather(key_second, "sp", axis=0, tiled=True),
        lax.all_gather(values, "sp", axis=0, tiled=True),
    )
    piece_rows = pieces[0].shape[0]
    key_pos = lax.broadcasted_iota(jnp.int32, (1, piece_rows), 1)
    allowed = key_pos <= query_pos
    value_rows = pieces[2].reshape(piece_rows, 2, heads_here, value_size)
    results = []
    for group_idx in range(2):
        key_width = key_widths[group_idx]
        key_part = pieces[group_idx].reshape(piece_rows, heads_here, 2, key_width)
        scores = jnp.einsum(
            "qhmd,khmd->hmqk", query_groups[group_idx], key_part, preferred_element_type=jnp.float32
        ) * key_width ** (-0.5)
        scores = jnp.where(allowed, scores, -1e30)
        running, totals, weighted = states[group_idx]
        new_peak = jnp.maximum(running, jnp.max(scores, axis=-1, keepdims=True))
        weights = jnp.where(allowed, jnp.exp(scores - new_peak), 0.0)
        totals = jnp.sum(weights, axis=-1, keepdims=True)
        weighted = jnp.einsum(
            "hmqk,khe->hmqe",
            weights.astype(jnp.bfloat16),
            value_rows[:, group_idx],
            preferred_element_type=jnp.float32,
        )
        results.append((new_peak, totals, weighted))
    states = (results[0], results[1])
    map_out = jnp.stack([states[0][2] / states[0][1], states[1][2] / states[1][1]])
    differ = map_out[:, :, 0] - lambdas[:, :, None, None] * map_out[:, :, 1]
    head_scale = lax.rsqrt(jnp.mean(differ * differ, axis=-1, keepdims=True) + 1e-06)
    attended = (0.8 * differ * head_scale).astype(jnp.bfloat16)
    projection = out_weight.reshape(2, heads_here, value_size, out_weight.shape[2])
    mixed_part = jnp.einsum(
        "ghqe,gher->qr", attended, projection, preferred_element_type=jnp.float32
    )
    mixed = lax.psum_scatter(
        mixed_part.astype(jnp.bfloat16), "tp", scatter_dimension=1, tiled=True
    ).astype(jnp.float32)
    stream = residual.astype(jnp.float32) + mixed
    squares = lax.psum(jnp.sum(stream * stream, axis=1), "tp")
    row_scale = lax.rsqrt(squares[:, None] / D + 1e-06)
    normed = (stream * row_scale * norm_gain.astype(jnp.float32)).astype(jnp.bfloat16)
    full_rows = lax.all_gather(normed, "tp", axis=1, tiled=True)
    pieces = (
        lax.all_gather(gate_weight, "sp", axis=0, tiled=True),
        lax.all_gather(up_weight, "sp", axis=0, tiled=True),
    )
    gate = jnp.dot(full_rows, pieces[0], preferred_element_type=jnp.float32)
    up_part = jnp.dot(full_rows, pieces[1], preferred_element_type=jnp.float32)
    hidden = (jax.nn.silu(gate) * up_part).astype(jnp.bfloat16)
    partial_out = jnp.dot(
        hidden,
        lax.all_gather(down_weight, "sp", axis=1, tiled=True),
        preferred_element_type=jnp.float32,
    )
    ffn = lax.psum_scatter(
        partial_out.astype(jnp.bfloat16), "tp", scatter_dimension=1, tiled=True
    ).astype(jnp.float32)
    return (stream + 0.5 * ffn).astype(jnp.bfloat16)


def shift(array, step, count):
    return lax.ppermute(array, "sp", [(i, (i + step) % count) for i in range(count)])


def swap(array, mask, count):
    return lax.ppermute(array, "tp", [(i, i ^ mask) for i in range(count)])


def swap_masks(count):
    masks = []
    while count > 1:
        count //= 2
        masks.append(count)
    return masks


def gather_swapped(array, axis, count):
    order = [0]
    for mask in swap_masks(count):
        array = jnp.concatenate([array, swap(array, mask, count)], axis=axis)
        order = order + [m ^ mask for m in order]
    return array, order


def pick(stack, index):
    return lax.dynamic_index_in_dim(stack, index, 0, keepdims=False)


def exchanged_weights(
    query_first,
    key_first,
    query_second,
    key_second,
    values,
    lambdas,
    residual,
    norm_gain,
    out_weight,
    gate_weight,
    up_weight,
    down_weight,
):
    n_sp = lax.axis_size("sp")
    n_tp = lax.axis_size("tp")
    s = lax.axis_index("sp")
    t = lax.axis_index("tp")
    tok_rows = query_first.shape[0]
    heads_here = lambdas.shape[1]
    value_size = values.shape[2] // heads_here
    model = out_weight.shape[2]

    own_kv = jnp.concatenate(
        [key_first, key_second, values.reshape(tok_rows, -1)], axis=1
    )
    kv_blocks = [own_kv] + [
        lax.ppermute(own_kv, "sp", [(i, i + d) for i in range(n_sp - d)])
        for d in range(1, n_sp)
    ]
    kv = jnp.concatenate(kv_blocks, axis=0)

    kv, out_weight, residual, gate_weight, up_weight, down_weight = lax.optimization_barrier(
        (kv, out_weight, residual, gate_weight, up_weight, down_weight)
    )
    ow_all, order = gather_swapped(
        out_weight.reshape(-1, model), 0, n_tp
    )
    res_rows = jnp.concatenate(
        [residual] + [shift(residual, d, n_sp) for d in range(1, n_sp)]
        + [jnp.broadcast_to(norm_gain[None, :], (16, norm_gain.shape[0]))],
        axis=0,
    )
    all_rows = tok_rows * n_sp
    res_all, _ = gather_swapped(res_rows[None], 0, n_tp)
    inverse = jnp.asarray([order.index(m) for m in range(n_tp)], jnp.int32)
    res_cols = jnp.concatenate(
        [pick(res_all, inverse[m ^ t]) for m in range(n_tp)], axis=1
    )
    residual_all = res_cols[:all_rows]
    gain_all = res_cols[all_rows : all_rows + 1].astype(jnp.float32)

    hid = gate_weight.shape[1]
    width = -(-hid // (n_sp * 128)) * 128
    starts = [min(j * width, hid - width) for j in range(n_sp)]
    gate_up = jnp.stack(
        [
            jnp.concatenate(
                [gate_weight[:, a : a + width], up_weight[:, a : a + width]], axis=1
            )
            for a in starts
        ]
    )
    down = jnp.stack([down_weight[a : a + width] for a in starts])
    gu_parts = []
    dn_parts = []
    for d in range(n_sp):
        gu = pick(gate_up, (s + d) % n_sp)
        dn = pick(down, (s + d) % n_sp)
        gu_parts.append(gu if d == 0 else shift(gu, d, n_sp))
        dn_parts.append(dn if d == 0 else shift(dn, d, n_sp))
    gu_stack = jnp.stack(gu_parts)
    dn_stack = jnp.stack(dn_parts)
    gu_all = jnp.concatenate(
        [pick(gu_stack, (s - b) % n_sp) for b in range(n_sp)], axis=0
    )
    dn_all = jnp.concatenate(
        [pick(dn_stack, (s - b) % n_sp) for b in range(n_sp)], axis=1
    )
    cols = model // n_tp
    dn_tp = jnp.stack([dn_all[:, b * cols : (b + 1) * cols] for b in range(n_tp)])
    dn_rel = jnp.concatenate([pick(dn_tp, m ^ t) for m in order], axis=1)

    q_idx = lax.broadcasted_iota(jnp.int32, (tok_rows, all_rows), 0)
    k_idx = lax.broadcasted_iota(jnp.int32, (tok_rows, all_rows), 1)
    allowed = jnp.where(k_idx < tok_rows, k_idx <= q_idx, k_idx < (s + 1) * tok_rows)
    offset = 0
    value_start = key_first.shape[1] + key_second.shape[1]
    value_all = kv[:, value_start:].reshape(all_rows, 2, heads_here, value_size)
    outs = []
    for g, query in enumerate((query_first, query_second)):
        span = query.shape[1]
        width_g = span // (2 * heads_here)
        keys = kv[:, offset : offset + span].reshape(all_rows, heads_here, 2, width_g)
        offset += span
        scores = jnp.einsum(
            "qhmd,khmd->hmqk",
            query.reshape(tok_rows, heads_here, 2, width_g),
            keys,
            preferred_element_type=jnp.float32,
        ) * width_g ** (-0.5)
        scores = jnp.where(allowed, scores, -1e30)
        peak = jnp.max(scores, axis=-1, keepdims=True)
        weights = jnp.where(allowed, jnp.exp(scores - peak), 0.0)
        totals = jnp.sum(weights, axis=-1, keepdims=True)
        weighted = jnp.einsum(
            "hmqk,khe->hmqe",
            weights.astype(jnp.bfloat16),
            value_all[:, g],
            preferred_element_type=jnp.float32,
        )
        outs.append(weighted / totals)
    map_out = jnp.stack(outs)
    differ = map_out[:, :, 0] - lambdas[:, :, None, None] * map_out[:, :, 1]
    head_scale = lax.rsqrt(jnp.mean(differ * differ, axis=-1, keepdims=True) + 1e-06)
    attended = (0.8 * differ * head_scale).astype(jnp.bfloat16)
    attended = attended.transpose(2, 0, 1, 3).reshape(tok_rows, -1)

    att_rows = jnp.concatenate(
        [attended] + [shift(attended, d, n_sp) for d in range(1, n_sp)], axis=0
    )
    att_all, _ = gather_swapped(att_rows, 1, n_tp)
    stream = residual_all.astype(jnp.float32) + jnp.dot(
        att_all, ow_all, preferred_element_type=jnp.float32
    )
    row_scale = lax.rsqrt(jnp.mean(stream * stream, axis=1, keepdims=True) + 1e-06)
    normed = (stream * row_scale * gain_all).astype(jnp.bfloat16)
    own_stream = lax.dynamic_slice(stream[:tok_rows], (0, t * cols), (tok_rows, cols))

    unit = lax.broadcasted_iota(jnp.int32, (1, width), 1)
    first_new = s * width - jnp.minimum(s * width, hid - width)
    fresh = unit >= first_new
    total = None
    for d in list(range(1, n_sp)) + [0]:
        both = jnp.dot(
            normed[d * tok_rows : (d + 1) * tok_rows], gu_all,
            preferred_element_type=jnp.float32,
        )
        hidden = jax.nn.silu(both[:, :width]) * both[:, width:]
        hidden = jnp.where(fresh, hidden, 0.0).astype(jnp.bfloat16)
        part = jnp.dot(hidden, dn_rel, preferred_element_type=jnp.float32)
        for mask in reversed(swap_masks(n_tp)):
            half = part.shape[1] // 2
            part = part[:, :half] + swap(
                part[:, half:].astype(jnp.bfloat16), mask, n_tp
            ).astype(jnp.float32)
        if d > 0:
            part = shift(part.astype(jnp.bfloat16), -d, n_sp).astype(jnp.float32)
        total = part if total is None else total + part
    return (own_stream + 0.5 * total).astype(jnp.bfloat16)


def per_device(*arrays):
    all_rows = arrays[0].shape[0] * lax.axis_size("sp")
    if all_rows < arrays[9].shape[1]:
        return exchanged_weights(*arrays)
    return gathered_weights(*arrays)


def solution(mesh):
    return jax.shard_map(
        per_device,
        mesh=mesh,
        in_specs=(
            P(("grp", "sp"), "tp"),
            P(("grp", "sp"), "tp"),
            P(("grp", "sp"), "tp"),
            P(("grp", "sp"), "tp"),
            P(("grp", "sp"), None, "tp"),
            P(None, "tp"),
            P(("grp", "sp"), "tp"),
            P("tp"),
            P(None, "tp", None),
            P("sp", "tp"),
            P("sp", "tp"),
            P("tp", "sp"),
        ),
        out_specs=P(("grp", "sp"), "tp"),
        check_vma=False,
    )
```
